32 devices in a mesh: sp: 8 (over z, y), tp: 4 (over x, core).
Axes of the slice: x: 2, y: 2, z: 4, core: 2. Of those that a mesh axis runs over, the one named last changes fastest.
Arguments:
- b_gate: bfloat16 [4096, 2048], P('sp', 'tp'), may hold values from -6 to 6
- c_gate: bfloat16 [4096, 2048], P('sp', 'tp'), may hold values from -6 to 6
- values_in: bfloat16 [4096, 2048], P('sp', 'tp'), may hold values from -6 to 6
- conv_taps: float32 [3, 2048], P(None, 'tp'), may hold values from -4 to 4
- out_proj: bfloat16 [2048, 2048], P('tp'), may hold values from -0.125 to 0.125
- resid: bfloat16 [4096, 2048], P(('sp', 'tp')), may hold values from -6 to 6
- post_gain: float32 [2048], replicated, may hold values from 0.1 to 1.9
- pre_gain: float32 [2048], replicated, may hold values from 0.1 to 1.9
- moe_gain: float32 [2048], replicated, may hold values from 0.1 to 1.9
- routes: int32 [4096, 4], P(('sp', 'tp')), may hold values from 0 to 7, all different within a row; in each aligned block of 128 rows (0 to 127, 128 to 255, ...) at most 128 rows name the same one
- route_weight: float32 [4096, 4], P(('sp', 'tp')), may hold values from 0.1 to 1
- gate_w: bfloat16 [8, 2048, 640], P('sp'), may hold values from -1 to 1
- up_w: bfloat16 [8, 2048, 640], P('sp'), may hold values from -1 to 1
- down_w: bfloat16 [8, 640, 2048], P('sp'), may hold values from -0.25 to 0.25
Outputs:
- result: bfloat16 [4096, 2048], P(('sp', 'tp'))
The draws below stay inside these ranges and needn't reach their ends.
Inputs may be any that keep to these rules, and one draw needn't show every extreme that they name: `routes`: each row names 4 different experts; within each aligned block of 128 rows no expert is named by more than 128 rows.
All inputs are finite; a program needn't handle non-finite values.
Results may differ from the reference program's by a relative error of at most 0.007.
Values may be sent and summed in bfloat16 or wider, within the bound.
No kernel may reach another device: no remote copies, remote signals or barrier semaphores. Data moves between devices by JAX's collectives and lax.ppermute only.
A program may use at most 64 MiB of HBM per device.

```python
import math
import jax
import jax.numpy as jnp
import numpy as np
from jax import lax

D = 2048
FF = 640
TOPK = 4
ROWS = 128
TOKENS = 4096
EXPERTS = 8
CAP = 128
N_SP = 8
N_TP = 4


def expert_matrix(key):
    scale = D ** (-0.5)
    sample = jax.random.normal(key, (EXPERTS, D, FF), jnp.float32) * scale
    return jnp.clip(sample, -1.0, 1.0).astype(jnp.bfloat16)


def draw_gate_w(key, part):
    return expert_matrix(jax.random.fold_in(key, 11))


def draw_up_w(key, part):
    return expert_matrix(jax.random.fold_in(key, 23))


def steps_of(stream_key, extent, pieces, low, largest):
    level, own = 1.0, jax.random.fold_in(stream_key, 6)
    for position, blocks in pieces:
        heights = jnp.exp(jax.random.uniform(jax.random.fold_in(own, position), (blocks,), jnp.float32, low / len(pieces), largest / len(pieces)))
        level = level * jnp.repeat(heights, extent[position] // blocks).reshape([-1 if axis == position else 1 for axis in range(len(extent))])
    return level


def deal_out(stream_key, own, number, rows, number_of, top, most, lean):
    ranking = jax.random.permutation(stream_key, number_of)
    crowded, ordinary = shares(number_of, rows * top, most, lean, True), shares(number_of, rows * top, most, lean, False)
    places = jnp.arange(number_of)

    def named(lengths, offset_by):
        used = int((lengths > 0).sum())
        fixed = max(1, used // 4)
        passed = fixed + (places - fixed + offset_by * (used - fixed)) % max(1, number_of - fixed)
        return jnp.zeros((number_of,), jnp.int32).at[ranking[jnp.where(places < fixed, places, passed)]].set(jnp.asarray(lengths, jnp.int32))

    lengths = jnp.where(number % 4 == 0, named(crowded, number // 4), named(ordinary, number - number // 4 - 1))
    mixed = jax.random.permutation(jax.random.fold_in(own, 3), number_of)
    source_of, sink = mixed[0:number_of // 2 * 2:2], mixed[1:number_of // 2 * 2:2]
    margin = jnp.minimum(lengths[source_of] - 1, most - lengths[sink]) // 2
    margin = jnp.where((source_of == ranking[0]) | (sink == ranking[0]) | (lengths[sink] == 0), 0, jnp.maximum(margin, 0))
    passed = jax.random.randint(jax.random.fold_in(own, 4), (number_of // 2,), 0, 1 << 20) % (margin + 1)
    lengths = lengths.at[source_of].add(-passed).at[sink].add(passed)
    labels = jnp.searchsorted(jnp.cumsum(lengths), jnp.arange(rows * top), side="right").astype(jnp.int32)
    listing = labels.reshape(top, rows).T
    listing = listing[jax.random.permutation(jax.random.fold_in(own, 1), rows)]
    offset_by = jax.random.randint(jax.random.fold_in(own, 2), (rows, 1), 0, top)
    return jnp.take_along_axis(listing, (jnp.arange(top)[None, :] + offset_by) % top, axis=1)


def shares(amount, total, most, skew, full):
    portions = [(1 << 20) // math.isqrt(standing ** skew) + 1 for standing in range(1, amount + 1)]
    largest = most if full else min(most, max(-(-total // amount), total * portions[0] // sum(portions)))
    least = 1 if total - largest >= amount - 1 else 0
    holding, surplus = [largest] + [least] * (amount - 1), total - largest - least * (amount - 1)
    while surplus > 0:
        free = [i for i in range(1, amount) if holding[i] < largest] or [i for i in range(1, amount) if holding[i] < most]
        mass, budget = sum([portions[i] for i in free]), surplus
        for i in free:
            more = min(most - holding[i], max(1, budget * portions[i] // mass), surplus)
            holding[i] = holding[i] + more
            surplus = surplus - more
    return np.array(holding)


def bell_draw(key, extent, width, most, cuts=(), kind=jnp.bfloat16):
    drawn = jax.random.normal(key, extent, jnp.float32) * width
    if len(cuts) > 0:
        drawn = steps_of(key, extent, cuts, -0.22, 0.18) * drawn
    return jnp.clip(drawn, min=-most, max=most).astype(kind)


def setup_inputs(seed: int = 0) -> dict:
    arg_keys = jax.random.split(jax.random.key(seed), 15)
    b_gate = bell_draw(arg_keys[0], (TOKENS, D), 1.0, 6.0, ((0, 8), (1, 4)))
    c_gate = bell_draw(arg_keys[1], (TOKENS, D), 1.0, 6.0, ((0, 8), (1, 4)))
    values_in = bell_draw(arg_keys[2], (TOKENS, D), 1.0, 6.0, ((0, 8), (1, 4)))
    conv_taps = bell_draw(arg_keys[3], (3, D), 0.577, 4.0, ((1, 4),), jnp.float32)
    out_proj = bell_draw(arg_keys[4], (D, D), D ** -0.5, 0.125, ((0, 4),))
    resid = bell_draw(arg_keys[5], (TOKENS, D), 1.0, 6.0, ((0, 32),))
    post_gain = jnp.clip(1.0 + 0.18 * jax.random.normal(arg_keys[6], (D,), jnp.float32), 0.1, 1.9)
    pre_gain = jnp.clip(1.0 + 0.18 * jax.random.normal(arg_keys[7], (D,), jnp.float32), 0.1, 1.9)
    moe_gain = jnp.clip(1.0 + 0.18 * jax.random.normal(arg_keys[8], (D,), jnp.float32), 0.1, 1.9)
    routes_keys = jax.random.split(jax.random.fold_in(arg_keys[9], 1), TOKENS // ROWS)
    routes_turns = jax.random.permutation(jax.random.fold_in(arg_keys[9], 3), TOKENS // ROWS)
    routes = jax.vmap(lambda own, number: deal_out(jax.random.fold_in(arg_keys[9], 2), own, number, ROWS, EXPERTS, TOPK, CAP, 1))(routes_keys, routes_turns).reshape((TOKENS, TOPK))
    route_weight = jnp.clip(0.1 + 0.9 * jax.random.uniform(arg_keys[10], (TOKENS, TOPK), jnp.float32) ** steps_of(arg_keys[10], (TOKENS, TOPK), ((0, 32),), -0.2, 0.2), 0.1, 1.0)
    gate_w = draw_gate_w(jax.random.fold_in(arg_keys[14], 71), 0)
    up_w = draw_up_w(jax.random.fold_in(arg_keys[14], 71), 0)
    down_w = bell_draw(arg_keys[13], (EXPERTS, FF, D), FF ** -0.5, 0.25, ((0, 8),))
    return {"b_gate": b_gate, "c_gate": c_gate, "values_in": values_in, "conv_taps": conv_taps, "out_proj": out_proj, "resid": resid, "post_gain": post_gain, "pre_gain": pre_gain, "moe_gain": moe_gain, "routes": routes, "route_weight": route_weight, "gate_w": gate_w, "up_w": up_w, "down_w": down_w}


epsilon = 1e-06

def rms_norm(vector, gain):
    return vector * lax.rsqrt(lax.optimization_barrier(jnp.mean(vector * vector, axis=-1, keepdims=True)) + epsilon) * gain

def reference(b_gate, c_gate, values_in, conv_taps, out_proj, resid, post_gain, pre_gain, moe_gain, routes, route_weight, gate_w, up_w, down_w):
    length = b_gate.shape[0]
    product = c_gate.astype(jnp.float32) * values_in.astype(jnp.float32)
    padded = jnp.pad(product, ((2, 0), (0, 0)))
    filtered = padded[0:length] * conv_taps[0] + padded[1:length + 1] * conv_taps[1] + padded[2:length + 2] * conv_taps[2]
    mixed = (b_gate.astype(jnp.float32) * filtered).astype(jnp.bfloat16)
    projected = jnp.dot(mixed, out_proj, preferred_element_type=jnp.float32)
    stream = (resid.astype(jnp.float32) + rms_norm(projected, post_gain)).astype(jnp.bfloat16)
    normed = rms_norm(stream.astype(jnp.float32), pre_gain).astype(jnp.bfloat16)
    flat_ids = routes.reshape(-1).astype(jnp.int32)
    flat_weight = route_weight.reshape(-1)
    assigned = flat_ids.shape[0]
    order = jnp.argsort(flat_ids, stable=True).astype(jnp.int32)
    counts = jnp.bincount(flat_ids, length=EXPERTS).astype(jnp.int32)
    starts = (jnp.cumsum(counts) - counts).astype(jnp.int32)
    bound = CAP * N_SP * N_TP
    offsets = jnp.arange(bound, dtype=jnp.int32)

    def one_expert(total, expert_id):
        positions = jnp.minimum(starts[expert_id] + offsets, assigned - 1).astype(jnp.int32)
        valid = (offsets < counts[expert_id]).astype(jnp.float32)
        picked = order[positions]
        token_ids = (picked // TOPK).astype(jnp.int32)
        rows_in = normed[token_ids]
        gate_pre = jnp.dot(rows_in, gate_w[expert_id], preferred_element_type=jnp.float32)
        up_pre = jnp.dot(rows_in, up_w[expert_id], preferred_element_type=jnp.float32)
        gate_act = jnp.minimum(gate_pre, 7.0)
        up_act = jnp.clip(up_pre, -7.0, 7.0)
        hidden = (gate_act * jax.nn.sigmoid(1.702 * gate_act) * (up_act + 1.0)).astype(jnp.bfloat16)
        expert_out = jnp.dot(hidden, down_w[expert_id], preferred_element_type=jnp.float32).astype(jnp.bfloat16)
        scaled = expert_out.astype(jnp.float32) * (flat_weight[picked] * valid)[:, None]
        return (total.at[token_ids].add(scaled), None)
    combined, _ = lax.scan(one_expert, jnp.zeros((length, D), jnp.float32), jnp.arange(EXPERTS, dtype=jnp.int32))
    return (stream.astype(jnp.float32) + rms_norm(combined, moe_gain)).astype(jnp.bfloat16)
```

```python
import jax
import jax.numpy as jnp
from jax import lax
from jax.sharding import PartitionSpec as P

epsilon = 1e-06


def shifted(shard, axis, by):
    devices = lax.axis_size(axis)
    pairs = [(i, i + by) for i in range(devices) if 0 <= i + by < devices]
    return lax.ppermute(shard, axis, pairs)


def rms_norm(vector, gain):
    return vector * lax.rsqrt(jnp.mean(vector * vector, axis=-1, keepdims=True) + epsilon) * gain


def ring_order(count):
    return list(range(0, count, 2)) + list(range(count - 1, 0, -2))


def swapped(shard, axis, flip):
    devices = lax.axis_size(axis)
    return lax.ppermute(shard, axis, [(i, i ^ flip) for i in range(devices)])


def scatter_sum(partial, axis):
    devices = lax.axis_size(axis)
    blocks = partial.reshape(devices, partial.shape[0] // devices, partial.shape[1])
    index = lax.axis_index(axis)
    flip = 1
    while flip < devices:
        pairs = blocks.reshape(blocks.shape[0] // 2, 2, *blocks.shape[1:])
        mine = (index // flip) % 2
        low, high = pairs[:, 0], pairs[:, 1]
        keep = jnp.where(mine == 0, low, high)
        give = jnp.where(mine == 0, high, low).astype(jnp.bfloat16)
        blocks = keep + swapped(give, axis, flip).astype(jnp.float32)
        flip *= 2
    return blocks[0]


def expert_rows(rows, weight, gate_w, up_w, down_w):
    gate_pre = jnp.dot(rows, gate_w, preferred_element_type=jnp.float32)
    up_pre = jnp.dot(rows, up_w, preferred_element_type=jnp.float32)
    gate_act = jnp.minimum(gate_pre, 7.0)
    up_act = jnp.clip(up_pre, -7.0, 7.0)
    hidden = (gate_act * jax.nn.sigmoid(1.702 * gate_act) * (up_act + 1.0)).astype(jnp.bfloat16)
    return jnp.dot(hidden, down_w, preferred_element_type=jnp.float32) * weight[:, None]


def ring_experts(normed, routes, route_weight, gate_w, up_w, down_w):
    devices = lax.axis_size("sp")
    own_count = normed.shape[0]
    order = ring_order(devices)
    place_of = [order.index(i) for i in range(devices)]
    ahead = [(order[i], order[(i + 1) % devices]) for i in range(devices)]
    behind = [(order[(i + 1) % devices], order[i]) for i in range(devices)]
    match = routes[:, :, None] == jnp.arange(devices, dtype=jnp.int32)[None, None, :]
    dense = jnp.sum(jnp.where(match, route_weight[:, :, None], 0.0), axis=1)
    table = lax.all_to_all(dense.T, "sp", split_axis=0, concat_axis=0, tiled=True)
    place = jnp.asarray(place_of, jnp.int32)[lax.axis_index("sp")]
    around = jnp.asarray(order, jnp.int32)[(place + jnp.arange(devices, dtype=jnp.int32)) % devices]
    table = table[around]
    far = devices // 2
    cut = own_count // 2

    def run(rows, weight):
        return expert_rows(rows, weight, gate_w[0], up_w[0], down_w[0])

    forth, back = normed, normed
    kept = {}
    for step in range(1, far):
        forth = lax.ppermute(forth, "sp", ahead)
        back = lax.ppermute(back, "sp", behind)
        out = run(
            jnp.concatenate([forth, back], axis=0),
            jnp.concatenate([table[devices - step], table[step]], axis=0),
        )
        kept[-step], kept[step] = out[:own_count], out[own_count:]
    forth = lax.ppermute(forth[:cut], "sp", ahead)
    back = lax.ppermute(back[cut:], "sp", behind)
    out = run(jnp.concatenate([forth, back], axis=0), table[far])
    to_ahead = lax.ppermute(out[:cut].astype(jnp.bfloat16), "sp", ahead)
    to_behind = lax.ppermute(out[cut:].astype(jnp.bfloat16), "sp", behind)
    own = run(normed, table[0])
    for step in range(far - 1, 0, -1):
        if step == far - 1:
            head = kept[step][:cut] + to_ahead.astype(jnp.float32)
            up = jnp.concatenate([head, kept[step][cut:]], axis=0)
            tail = kept[-step][cut:] + to_behind.astype(jnp.float32)
            down = jnp.concatenate([kept[-step][:cut], tail], axis=0)
        else:
            up = kept[step] + to_ahead.astype(jnp.float32)
            down = kept[-step] + to_behind.astype(jnp.float32)
        to_ahead = lax.ppermute(up.astype(jnp.bfloat16), "sp", ahead)
        to_behind = lax.ppermute(down.astype(jnp.bfloat16), "sp", behind)
    return own + to_ahead.astype(jnp.float32) + to_behind.astype(jnp.float32)


def exchange_experts(normed, routes, route_weight, gate_w, up_w, down_w):
    own_count = normed.shape[0]
    width = normed.shape[1]
    top_count = routes.shape[1]
    experts = lax.axis_size("sp")
    capacity = 2 * own_count * top_count // experts
    flat_ids = routes.reshape(-1)
    assigned = flat_ids.shape[0]
    onehot = (flat_ids[:, None] == jnp.arange(experts, dtype=jnp.int32)[None, :]).astype(jnp.int32)
    earlier = jnp.cumsum(onehot, axis=0) - onehot
    slot_index = jnp.sum(earlier * onehot, axis=1)
    target = flat_ids * capacity + slot_index
    source = (
        jnp.full((experts * capacity,), assigned, jnp.int32)
        .at[target]
        .set(jnp.arange(assigned, dtype=jnp.int32))
    )
    row_index = jnp.where(source < assigned, source // top_count, own_count)
    with_blank = jnp.concatenate([normed, jnp.zeros((1, width), jnp.bfloat16)], axis=0)
    outgoing = with_blank[row_index].reshape(experts, capacity, width)
    slots_in = lax.all_to_all(outgoing, "sp", split_axis=0, concat_axis=0, tiled=True)
    gate_pre = jnp.dot(slots_in, gate_w[0], preferred_element_type=jnp.float32)
    up_pre = jnp.dot(slots_in, up_w[0], preferred_element_type=jnp.float32)
    gate_act = jnp.minimum(gate_pre, 7.0)
    up_act = jnp.clip(up_pre, -7.0, 7.0)
    hidden = (gate_act * jax.nn.sigmoid(1.702 * gate_act) * (up_act + 1.0)).astype(jnp.bfloat16)
    expert_out = jnp.dot(hidden, down_w[0], preferred_element_type=jnp.float32).astype(jnp.bfloat16)
    returned = lax.all_to_all(expert_out, "sp", split_axis=0, concat_axis=0, tiled=True)
    chosen = returned.reshape(experts * capacity, width)[target].astype(jnp.float32)
    weighted = chosen * route_weight.reshape(-1)[:, None]
    return jnp.sum(weighted.reshape(own_count, top_count, width), axis=1)


def body(
    b_gate,
    c_gate,
    values_in,
    conv_taps,
    out_proj,
    resid,
    post_gain,
    pre_gain,
    moe_gain,
    routes,
    route_weight,
    gate_w,
    up_w,
    down_w,
):
    tok_rows = b_gate.shape[0]
    product = c_gate.astype(jnp.float32) * values_in.astype(jnp.float32)
    prior_rows = shifted(product[tok_rows - 2 :], "sp", 1)
    padded = jnp.concatenate([prior_rows, product], axis=0)
    filtered = (
        padded[0:tok_rows] * conv_taps[0]
        + padded[1 : tok_rows + 1] * conv_taps[1]
        + padded[2 : tok_rows + 2] * conv_taps[2]
    )
    mixed_rows = (b_gate.astype(jnp.float32) * filtered).astype(jnp.bfloat16)
    projected = scatter_sum(jnp.dot(mixed_rows, out_proj, preferred_element_type=jnp.float32), "tp")
    stream = (resid.astype(jnp.float32) + rms_norm(projected, post_gain)).astype(jnp.bfloat16)
    normed = rms_norm(stream.astype(jnp.float32), pre_gain).astype(jnp.bfloat16)
    spread = lax.axis_size("sp") * routes.shape[0]
    padded_slots = 2 * routes.shape[0] * routes.shape[1]
    plan = ring_experts if padded_slots >= spread else exchange_experts
    combined = plan(normed, routes, route_weight, gate_w, up_w, down_w)
    return (stream.astype(jnp.float32) + rms_norm(combined, moe_gain)).astype(jnp.bfloat16)


def solution(mesh):
    placed = (
        P("sp", "tp"),
        P("sp", "tp"),
        P("sp", "tp"),
        P(None, "tp"),
        P("tp", None),
        P(("sp", "tp"), None),
        P(),
        P(),
        P(),
        P(("sp", "tp"), None),
        P(("sp", "tp"), None),
        P("sp", None, None),
        P("sp", None, None),
        P("sp", None, None),
    )
    return jax.shard_map(
        body, mesh=mesh, in_specs=placed, out_specs=P(("sp", "tp"), None), check_vma=False
    )
```

```python
import jax
import jax.numpy as jnp
from jax import lax
from jax.experimental import pallas as pl
from jax.experimental.pallas import tpu as pltpu
from jax.sharding import PartitionSpec as P

epsilon = 1e-06


def shifted(shard, axis, by):
    devices = lax.axis_size(axis)
    pairs = [(i, i + by) for i in range(devices) if 0 <= i + by < devices]
    return lax.ppermute(shard, axis, pairs)


def rms_norm(vector, gain):
    return vector * lax.rsqrt(jnp.mean(vector * vector, axis=-1, keepdims=True) + epsilon) * gain


def ring_order(count):
    return list(range(0, count, 2)) + list(range(count - 1, 0, -2))


def swapped(shard, axis, flip):
    devices = lax.axis_size(axis)
    return lax.ppermute(shard, axis, [(i, i ^ flip) for i in range(devices)])


def scatter_sum(partial, axis, cuts):
    devices = lax.axis_size(axis)
    blocks = partial.reshape(devices, partial.shape[0] // devices, partial.shape[1])
    index = lax.axis_index(axis)
    flip = 1
    while True:
        pairs = blocks.reshape(blocks.shape[0] // 2, 2, *blocks.shape[1:])
        mine = (index // flip) % 2
        low, high = pairs[:, 0], pairs[:, 1]
        keep = jnp.where(mine == 0, low, high)
        give = jnp.where(mine == 0, high, low).astype(jnp.bfloat16)
        if flip * 2 == devices:
            break
        blocks = keep + swapped(give, axis, flip).astype(jnp.float32)
        flip *= 2
    size = keep.shape[1] // cuts
    halves = [slice(i * size, (i + 1) * size) for i in range(cuts)]
    gives = [give[0, part] for part in halves]
    return [(keep[0, part], swapped(g, axis, flip)) for part, g in zip(halves, gives)], gives


def scaled(vector, gain):
    return vector * lax.rsqrt(jnp.mean(vector * vector, axis=-1, keepdims=True) + epsilon) * gain


def norm_kernel(keep, got, resid, post_gain, pre_gain, stream, normed):
    projected = keep[...] + got[...].astype(jnp.float32)
    rows = (resid[...].astype(jnp.float32) + scaled(projected, post_gain[...])).astype(jnp.bfloat16)
    stream[...] = rows
    normed[...] = scaled(rows.astype(jnp.float32), pre_gain[...]).astype(jnp.bfloat16)


def norm_rows(keep, got, resid, post_gain, pre_gain, place):
    size, width = keep.shape
    full = pl.BlockSpec((size, width), lambda i: (0, 0))
    gain = pl.BlockSpec((1, width), lambda i: (0, 0))
    shape = jax.ShapeDtypeStruct((size, width), jnp.bfloat16)
    return pl.pallas_call(
        norm_kernel,
        grid=(1,),
        in_specs=[full, full, pl.BlockSpec((size, width), lambda i: (place, 0)), gain, gain],
        out_specs=[full, full],
        out_shape=[shape, shape],
        name="norm_rows",
    )(keep, got, resid, post_gain[None], pre_gain[None])


def expert_call(parts, picks, table, gate_w, up_w, down_w):
    count, size, width = len(parts), parts[0].shape[0], parts[0].shape[1]
    hidden_width = gate_w.shape[2]
    block = 128 if hidden_width % 128 == 0 else hidden_width
    steps = hidden_width // block

    def kernel(*refs):
        ins, (weights, gate, up, down) = refs[:count], refs[count : count + 4]
        outs, (rows, total) = refs[count + 4 : 2 * count + 4], refs[2 * count + 4 :]
        step = pl.program_id(0)

        @pl.when(step == 0)
        def _():
            for i in range(count):
                rows[i * size : (i + 1) * size, :] = ins[i][...]
            total[...] = jnp.zeros_like(total)

        gate_pre = jnp.dot(rows[...], gate[0], preferred_element_type=jnp.float32)
        up_pre = jnp.dot(rows[...], up[0], preferred_element_type=jnp.float32)
        gate_act = jnp.minimum(gate_pre, 7.0)
        up_act = jnp.clip(up_pre, -7.0, 7.0)
        hidden = (gate_act * jax.nn.sigmoid(1.702 * gate_act) * (up_act + 1.0)).astype(jnp.bfloat16)
        total[...] += jnp.dot(hidden, down[0], preferred_element_type=jnp.float32)

        @pl.when(step == steps - 1)
        def _():
            for i, (first, column) in enumerate(picks):
                weight = weights[first : first + size, column : column + 1]
                outs[i][...] = (total[i * size : (i + 1) * size, :] * weight).astype(jnp.bfloat16)

    full = pl.BlockSpec((size, width), lambda i: (0, 0))
    return pl.pallas_call(
        kernel,
        grid=(steps,),
        in_specs=[full] * count
        + [
            pl.BlockSpec(table.shape, lambda i: (0, 0)),
            pl.BlockSpec((1, width, block), lambda i: (0, 0, i)),
            pl.BlockSpec((1, width, block), lambda i: (0, 0, i)),
            pl.BlockSpec((1, block, width), lambda i: (0, i, 0)),
        ],
        out_specs=[full] * count,
        out_shape=[jax.ShapeDtypeStruct((size, width), jnp.bfloat16)] * count,
        scratch_shapes=[
            pltpu.VMEM((count * size, width), jnp.bfloat16),
            pltpu.VMEM((count * size, width), jnp.float32),
        ],
        cost_estimate=pl.CostEstimate(
            flops=6 * count * size * width * hidden_width,
            bytes_accessed=6 * width * hidden_width + 4 * count * size * width,
            transcendentals=count * size * hidden_width,
        ),
        name="expert_rows",
    )(*parts, table, gate_w, up_w, down_w)


def finish_kernel(own_a, ahead_a, behind_a, own_b, ahead_b, behind_b, stream_a, stream_b, gain, out):
    size = own_a.shape[0]
    for i, (own, ahead, behind, stream) in enumerate(
        ((own_a, ahead_a, behind_a, stream_a), (own_b, ahead_b, behind_b, stream_b))
    ):
        combined = own[...].astype(jnp.float32) + ahead[...].astype(jnp.float32)
        combined = combined + behind[...].astype(jnp.float32)
        rows = stream[...].astype(jnp.float32) + scaled(combined, gain[...])
        out[i * size : (i + 1) * size, :] = rows.astype(jnp.bfloat16)


def finish(sums, streams, gain):
    size, width = streams[0].shape
    return pl.pallas_call(
        finish_kernel,
        out_shape=jax.ShapeDtypeStruct((2 * size, width), jnp.bfloat16),
        name="finish",
    )(*sums[0], *sums[1], *streams, gain[None])


def joined(kept, got):
    return (kept.astype(jnp.float32) + got.astype(jnp.float32)).astype(jnp.bfloat16)


def tied(array, *others):
    return lax.optimization_barrier((array, *others))[0]


def ring_table(routes, route_weight, after):
    devices = lax.axis_size("sp")
    order = ring_order(devices)
    place_of = [order.index(i) for i in range(devices)]
    match = routes[:, :, None] == jnp.arange(devices, dtype=jnp.int32)[None, None, :]
    dense = jnp.sum(jnp.where(match, route_weight[:, :, None], 0.0), axis=1)
    table = lax.all_to_all(tied(dense, *after).T, "sp", split_axis=0, concat_axis=0, tiled=True)
    place = jnp.asarray(place_of, jnp.int32)[lax.axis_index("sp")]
    around = jnp.asarray(order, jnp.int32)[(place + jnp.arange(devices, dtype=jnp.int32)) % devices]
    return table[around].T


def ring_experts(halves, table, gate_w, up_w, down_w):
    devices = lax.axis_size("sp")
    size = halves[0].shape[0]
    order = ring_order(devices)
    ahead = [(order[i], order[(i + 1) % devices]) for i in range(devices)]
    behind = [(order[(i + 1) % devices], order[i]) for i in range(devices)]
    far = devices // 2

    def run(parts, picks):
        return expert_call(parts, picks, table, gate_w, up_w, down_w)

    forth, back = list(halves), list(halves)
    own = run(halves, [(0, 0), (size, 0)])
    kept_up, kept_down = {}, {}
    done = {1: [], 2: own}
    for step in range(1, far):
        for h in (0, 1):
            forth[h] = lax.ppermute(tied(forth[h], *done[step]), "sp", ahead)
            back[h] = lax.ppermute(tied(back[h], *done[step]), "sp", behind)
        out = run(
            [forth[0], forth[1], back[0], back[1]],
            [(0, devices - step), (size, devices - step), (0, step), (size, step)],
        )
        done[step + 2] = out
        kept_down[step], kept_up[step] = out[:2], out[2:]
    first = lax.ppermute(tied(forth[0], *done[far]), "sp", ahead)
    last = lax.ppermute(tied(back[1], *done[far]), "sp", behind)
    far_out = run([first, last], [(0, far), (size, far)])
    up = [lax.ppermute(far_out[0], "sp", ahead), None]
    down = [None, lax.ppermute(far_out[1], "sp", behind)]
    for step in range(far - 1, 0, -1):
        for h in (0, 1):
            up_rows = kept_up[step][h] if up[h] is None else joined(kept_up[step][h], up[h])
            down_rows = kept_down[step][h] if down[h] is None else joined(kept_down[step][h], down[h])
            up[h] = lax.ppermute(up_rows, "sp", ahead)
            down[h] = lax.ppermute(down_rows, "sp", behind)
    return [(own[h], up[h], down[h]) for h in (0, 1)]


def exchange_experts(normed, routes, route_weight, gate_w, up_w, down_w):
    own_count = normed.shape[0]
    width = normed.shape[1]
    top_count = routes.shape[1]
    experts = lax.axis_size("sp")
    capacity = 2 * own_count * top_count // experts
    flat_ids = routes.reshape(-1)
    assigned = flat_ids.shape[0]
    onehot = (flat_ids[:, None] == jnp.arange(experts, dtype=jnp.int32)[None, :]).astype(jnp.int32)
    earlier = jnp.cumsum(onehot, axis=0) - onehot
    slot_index = jnp.sum(earlier * onehot, axis=1)
    target = flat_ids * capacity + slot_index
    source = (
        jnp.full((experts * capacity,), assigned, jnp.int32)
        .at[target]
        .set(jnp.arange(assigned, dtype=jnp.int32))
    )
    row_index = jnp.where(source < assigned, source // top_count, own_count)
    with_blank = jnp.concatenate([normed, jnp.zeros((1, width), jnp.bfloat16)], axis=0)
    outgoing = with_blank[row_index].reshape(experts, capacity, width)
    slots_in = lax.all_to_all(outgoing, "sp", split_axis=0, concat_axis=0, tiled=True)
    gate_pre = jnp.dot(slots_in, gate_w[0], preferred_element_type=jnp.float32)
    up_pre = jnp.dot(slots_in, up_w[0], preferred_element_type=jnp.float32)
    gate_act = jnp.minimum(gate_pre, 7.0)
    up_act = jnp.clip(up_pre, -7.0, 7.0)
    hidden = (gate_act * jax.nn.sigmoid(1.702 * gate_act) * (up_act + 1.0)).astype(jnp.bfloat16)
    expert_out = jnp.dot(hidden, down_w[0], preferred_element_type=jnp.float32).astype(jnp.bfloat16)
    returned = lax.all_to_all(expert_out, "sp", split_axis=0, concat_axis=0, tiled=True)
    chosen = returned.reshape(experts * capacity, width)[target].astype(jnp.float32)
    weighted = chosen * route_weight.reshape(-1)[:, None]
    return jnp.sum(weighted.reshape(own_count, top_count, width), axis=1)


def body(
    b_gate,
    c_gate,
    values_in,
    conv_taps,
    out_proj,
    resid,
    post_gain,
    pre_gain,
    moe_gain,
    routes,
    route_weight,
    gate_w,
    up_w,
    down_w,
):
    tok_rows = b_gate.shape[0]
    product = c_gate.astype(jnp.float32) * values_in.astype(jnp.float32)
    prior_rows = shifted(product[tok_rows - 2 :], "sp", 1)
    padded = jnp.concatenate([prior_rows, product], axis=0)
    filtered = (
        padded[0:tok_rows] * conv_taps[0]
        + padded[1 : tok_rows + 1] * conv_taps[1]
        + padded[2 : tok_rows + 2] * conv_taps[2]
    )
    mixed_rows = (b_gate.astype(jnp.float32) * filtered).astype(jnp.bfloat16)
    partial = jnp.dot(mixed_rows, out_proj, preferred_element_type=jnp.float32)
    pairs, given = scatter_sum(partial, "tp", 2)
    spread = lax.axis_size("sp") * routes.shape[0]
    ring = 2 * routes.shape[0] * routes.shape[1] >= spread
    table = ring_table(routes, route_weight, given) if ring else None
    streams, normed = [], []
    for place, (keep, got) in enumerate(pairs):
        keep = tied(keep, table) if ring else keep
        rows = norm_rows(keep, got, resid, post_gain, pre_gain, place)
        streams.append(rows[0])
        normed.append(rows[1])
    if ring:
        sums = ring_experts(normed, table, gate_w, up_w, down_w)
        return finish(sums, streams, moe_gain)
    stream = jnp.concatenate(streams, axis=0)
    normed = jnp.concatenate(normed, axis=0)
    combined = exchange_experts(normed, routes, route_weight, gate_w, up_w, down_w)
    return (stream.astype(jnp.float32) + rms_norm(combined, moe_gain)).astype(jnp.bfloat16)


def solution(mesh):
    placed = (
        P("sp", "tp"),
        P("sp", "tp"),
        P("sp", "tp"),
        P(None, "tp"),
        P("tp", None),
        P(("sp", "tp"), None),
        P(),
        P(),
        P(),
        P(("sp", "tp"), None),
        P(("sp", "tp"), None),
        P("sp", None, None),
        P("sp", None, None),
        P("sp", None, None),
    )
    return jax.shard_map(
        body, mesh=mesh, in_specs=placed, out_specs=P(("sp", "tp"), None), check_vma=False
    )
```

```python
import jax
import jax.numpy as jnp
from jax import lax
from jax.experimental import pallas as pl
from jax.experimental.pallas import tpu as pltpu
from jax.sharding import PartitionSpec as P

epsilon = 1e-06


def shifted(shard, axis, by):
    devices = lax.axis_size(axis)
    pairs = [(i, i + by) for i in range(devices) if 0 <= i + by < devices]
    return lax.ppermute(shard, axis, pairs)


def rms_norm(vector, gain):
    return vector * lax.rsqrt(jnp.mean(vector * vector, axis=-1, keepdims=True) + epsilon) * gain


def ring_order(count):
    return list(range(0, count, 2)) + list(range(count - 1, 0, -2))


def swapped(shard, axis, flip):
    devices = lax.axis_size(axis)
    return lax.ppermute(shard, axis, [(i, i ^ flip) for i in range(devices)])


def scatter_sum(partial, axis, cuts):
    devices = lax.axis_size(axis)
    blocks = partial.reshape(devices, partial.shape[0] // devices, partial.shape[1])
    index = lax.axis_index(axis)
    flip = 1
    while True:
        pairs = blocks.reshape(blocks.shape[0] // 2, 2, *blocks.shape[1:])
        mine = (index // flip) % 2
        low, high = pairs[:, 0], pairs[:, 1]
        keep = jnp.where(mine == 0, low, high)
        give = jnp.where(mine == 0, high, low).astype(jnp.bfloat16)
        if flip * 2 == devices:
            break
        blocks = keep.astype(jnp.float32) + swapped(give, axis, flip).astype(jnp.float32)
        flip *= 2
    size = keep.shape[1] // cuts
    halves = [slice(i * size, (i + 1) * size) for i in range(cuts)]
    gives = [give[0, part] for part in halves]
    return [(keep[0, part], swapped(g, axis, flip)) for part, g in zip(halves, gives)], gives


def scaled(vector, gain):
    return vector * lax.rsqrt(jnp.mean(vector * vector, axis=-1, keepdims=True) + epsilon) * gain


def norm_kernel(keep, got, resid, post_gain, pre_gain, stream, normed):
    projected = keep[...] + got[...].astype(jnp.float32)
    rows = (resid[...].astype(jnp.float32) + scaled(projected, post_gain[...])).astype(jnp.bfloat16)
    stream[...] = rows
    normed[...] = scaled(rows.astype(jnp.float32), pre_gain[...]).astype(jnp.bfloat16)


def norm_rows(keep, got, resid, post_gain, pre_gain, place):
    size, width = keep.shape
    full = pl.BlockSpec((size, width), lambda i: (0, 0))
    gain = pl.BlockSpec((1, width), lambda i: (0, 0))
    shape = jax.ShapeDtypeStruct((size, width), jnp.bfloat16)
    return pl.pallas_call(
        norm_kernel,
        grid=(1,),
        in_specs=[full, full, pl.BlockSpec((size, width), lambda i: (place, 0)), gain, gain],
        out_specs=[full, full],
        out_shape=[shape, shape],
        compiler_params=pltpu.CompilerParams(vmem_limit_bytes=24 * 1024 * 1024),
        name="norm_rows",
    )(keep, got, resid, post_gain[None], pre_gain[None])


def expert_call(parts, picks, table, gate_w, up_w, down_w):
    count, size, width = len(parts), parts[0].shape[0], parts[0].shape[1]
    hidden_width = gate_w.shape[2]
    block = 128 if hidden_width % 128 == 0 else hidden_width
    steps = hidden_width // block

    def kernel(*refs):
        ins, (weights, gate, up, down) = refs[:count], refs[count : count + 4]
        outs, (total,) = refs[count + 4 : 2 * count + 4], refs[2 * count + 4 :]
        rows = jnp.concatenate([ref[...] for ref in ins], axis=0)
        for step in range(steps):
            span = slice(step * block, (step + 1) * block)
            gate_pre = jnp.dot(rows, gate[0, :, span], preferred_element_type=jnp.float32)
            up_pre = jnp.dot(rows, up[0, :, span], preferred_element_type=jnp.float32)
            gate_act = jnp.minimum(gate_pre, 7.0)
            up_act = jnp.clip(up_pre, -7.0, 7.0)
            hidden = gate_act * jax.nn.sigmoid(1.702 * gate_act) * (up_act + 1.0)
            total[:, span] = hidden.astype(jnp.bfloat16)
        for i, (first, column) in enumerate(picks):
            weight = weights[first : first + size, column : column + 1]
            part = total[i * size : (i + 1) * size, :]
            out = jnp.dot(part, down[0], preferred_element_type=jnp.float32)
            outs[i][...] = (out * weight).astype(jnp.bfloat16)

    vmem = pl.BlockSpec(memory_space=pltpu.VMEM)
    held = [pltpu.with_memory_space_constraint(w, pltpu.VMEM) for w in (gate_w, up_w, down_w)]
    return pl.pallas_call(
        kernel,
        in_specs=[vmem] * (count + 4),
        out_specs=[vmem] * count,
        out_shape=[jax.ShapeDtypeStruct((size, width), jnp.bfloat16)] * count,
        scratch_shapes=[pltpu.VMEM((count * size, hidden_width), jnp.bfloat16)],
        cost_estimate=pl.CostEstimate(
            flops=6 * count * size * width * hidden_width,
            bytes_accessed=6 * width * hidden_width + 4 * count * size * width,
            transcendentals=count * size * hidden_width,
        ),
        compiler_params=pltpu.CompilerParams(vmem_limit_bytes=24 * 1024 * 1024),
        name="expert_rows",
    )(*parts, table, *held)


def finish_kernel(own_a, ahead_a, behind_a, own_b, ahead_b, behind_b, stream_a, stream_b, gain, out):
    size = own_a.shape[0]
    for i, (own, ahead, behind, stream) in enumerate(
        ((own_a, ahead_a, behind_a, stream_a), (own_b, ahead_b, behind_b, stream_b))
    ):
        combined = own[...].astype(jnp.float32) + ahead[...].astype(jnp.float32)
        combined = combined + behind[...].astype(jnp.float32)
        rows = stream[...].astype(jnp.float32) + scaled(combined, gain[...])
        out[i * size : (i + 1) * size, :] = rows.astype(jnp.bfloat16)


def finish(sums, streams, gain):
    size, width = streams[0].shape
    return pl.pallas_call(
        finish_kernel,
        out_shape=jax.ShapeDtypeStruct((2 * size, width), jnp.bfloat16),
        compiler_params=pltpu.CompilerParams(vmem_limit_bytes=24 * 1024 * 1024),
        name="finish",
    )(*sums[0], *sums[1], *streams, gain[None])


def joined(kept, got):
    return (kept.astype(jnp.float32) + got.astype(jnp.float32)).astype(jnp.bfloat16)


def tied(array, *others):
    return lax.optimization_barrier((array, *others))[0]


def ring_table(routes, route_weight, after):
    devices = lax.axis_size("sp")
    order = ring_order(devices)
    place_of = [order.index(i) for i in range(devices)]
    match = routes[:, :, None] == jnp.arange(devices, dtype=jnp.int32)[None, None, :]
    dense = jnp.sum(jnp.where(match, route_weight[:, :, None], 0.0), axis=1)
    table = lax.all_to_all(tied(dense, *after).T, "sp", split_axis=0, concat_axis=0, tiled=True)
    place = jnp.asarray(place_of, jnp.int32)[lax.axis_index("sp")]
    around = jnp.asarray(order, jnp.int32)[(place + jnp.arange(devices, dtype=jnp.int32)) % devices]
    return table[around].T


def ring_experts(halves, table, gate_w, up_w, down_w):
    devices = lax.axis_size("sp")
    size = halves[0].shape[0]
    order = ring_order(devices)
    ahead = [(order[i], order[(i + 1) % devices]) for i in range(devices)]
    behind = [(order[(i + 1) % devices], order[i]) for i in range(devices)]
    far = devices // 2

    def run(parts, picks):
        return expert_call(parts, picks, table, gate_w, up_w, down_w)

    forth, back = list(halves), list(halves)
    own = run(halves, [(0, 0), (size, 0)])
    kept_up, kept_down = {}, {}
    done = {1: [], 2: own}
    for step in range(1, far):
        for h in (0, 1):
            forth[h] = lax.ppermute(tied(forth[h], *done[step]), "sp", ahead)
            back[h] = lax.ppermute(tied(back[h], *done[step]), "sp", behind)
        out = run(
            [forth[0], forth[1], back[0], back[1]],
            [(0, devices - step), (size, devices - step), (0, step), (size, step)],
        )
        done[step + 2] = out
        kept_down[step], kept_up[step] = out[:2], out[2:]
    first = lax.ppermute(tied(forth[0], *done[far]), "sp", ahead)
    last = lax.ppermute(tied(back[1], *done[far]), "sp", behind)
    far_out = run([first, last], [(0, far), (size, far)])
    up = [lax.ppermute(far_out[0], "sp", ahead), None]
    down = [None, lax.ppermute(far_out[1], "sp", behind)]
    for step in range(far - 1, 0, -1):
        for h in (0, 1):
            up_rows = kept_up[step][h] if up[h] is None else joined(kept_up[step][h], up[h])
            down_rows = kept_down[step][h] if down[h] is None else joined(kept_down[step][h], down[h])
            up[h] = lax.ppermute(up_rows, "sp", ahead)
            down[h] = lax.ppermute(down_rows, "sp", behind)
    return [(own[h], up[h], down[h]) for h in (0, 1)]


def exchange_experts(normed, routes, route_weight, gate_w, up_w, down_w):
    own_count = normed.shape[0]
    width = normed.shape[1]
    top_count = routes.shape[1]
    experts = lax.axis_size("sp")
    capacity = 2 * own_count * top_count // experts
    flat_ids = routes.reshape(-1)
    assigned = flat_ids.shape[0]
    onehot = (flat_ids[:, None] == jnp.arange(experts, dtype=jnp.int32)[None, :]).astype(jnp.int32)
    earlier = jnp.cumsum(onehot, axis=0) - onehot
    slot_index = jnp.sum(earlier * onehot, axis=1)
    target = flat_ids * capacity + slot_index
    source = (
        jnp.full((experts * capacity,), assigned, jnp.int32)
        .at[target]
        .set(jnp.arange(assigned, dtype=jnp.int32))
    )
    row_index = jnp.where(source < assigned, source // top_count, own_count)
    with_blank = jnp.concatenate([normed, jnp.zeros((1, width), jnp.bfloat16)], axis=0)
    outgoing = with_blank[row_index].reshape(experts, capacity, width)
    slots_in = lax.all_to_all(outgoing, "sp", split_axis=0, concat_axis=0, tiled=True)
    gate_pre = jnp.dot(slots_in, gate_w[0], preferred_element_type=jnp.float32)
    up_pre = jnp.dot(slots_in, up_w[0], preferred_element_type=jnp.float32)
    gate_act = jnp.minimum(gate_pre, 7.0)
    up_act = jnp.clip(up_pre, -7.0, 7.0)
    hidden = (gate_act * jax.nn.sigmoid(1.702 * gate_act) * (up_act + 1.0)).astype(jnp.bfloat16)
    expert_out = jnp.dot(hidden, down_w[0], preferred_element_type=jnp.float32).astype(jnp.bfloat16)
    returned = lax.all_to_all(expert_out, "sp", split_axis=0, concat_axis=0, tiled=True)
    chosen = returned.reshape(experts * capacity, width)[target].astype(jnp.float32)
    weighted = chosen * route_weight.reshape(-1)[:, None]
    return jnp.sum(weighted.reshape(own_count, top_count, width), axis=1)


def body(
    b_gate,
    c_gate,
    values_in,
    conv_taps,
    out_proj,
    resid,
    post_gain,
    pre_gain,
    moe_gain,
    routes,
    route_weight,
    gate_w,
    up_w,
    down_w,
):
    tok_rows = b_gate.shape[0]
    product = c_gate.astype(jnp.float32) * values_in.astype(jnp.float32)
    prior_rows = shifted(product[tok_rows - 2 :], "sp", 1)
    padded = jnp.concatenate([prior_rows, product], axis=0)
    filtered = (
        padded[0:tok_rows] * conv_taps[0]
        + padded[1 : tok_rows + 1] * conv_taps[1]
        + padded[2 : tok_rows + 2] * conv_taps[2]
    )
    mixed_rows = (b_gate.astype(jnp.float32) * filtered).astype(jnp.bfloat16)
    partial = jnp.dot(mixed_rows, out_proj, preferred_element_type=jnp.float32).astype(jnp.bfloat16)
    pairs, given = scatter_sum(partial, "tp", 2)
    spread = lax.axis_size("sp") * routes.shape[0]
    ring = 2 * routes.shape[0] * routes.shape[1] >= spread
    table = ring_table(routes, route_weight, given) if ring else None
    streams, normed = [], []
    for place, (keep, got) in enumerate(pairs):
        keep = tied(keep, table) if ring and place == 1 else keep
        rows = norm_rows(keep, got, resid, post_gain, pre_gain, place)
        streams.append(rows[0])
        normed.append(rows[1])
    if ring:
        sums = ring_experts(normed, table, gate_w, up_w, down_w)
        return finish(sums, streams, moe_gain)
    stream = jnp.concatenate(streams, axis=0)
    normed = jnp.concatenate(normed, axis=0)
    combined = exchange_experts(normed, routes, route_weight, gate_w, up_w, down_w)
    return (stream.astype(jnp.float32) + rms_norm(combined, moe_gain)).astype(jnp.bfloat16)


def solution(mesh):
    placed = (
        P("sp", "tp"),
        P("sp", "tp"),
        P("sp", "tp"),
        P(None, "tp"),
        P("tp", None),
        P(("sp", "tp"), None),
        P(),
        P(),
        P(),
        P(("sp", "tp"), None),
        P(("sp", "tp"), None),
        P("sp", None, None),
        P("sp", None, None),
        P("sp", None, None),
    )
    return jax.shard_map(
        body, mesh=mesh, in_specs=placed, out_specs=P(("sp", "tp"), None), check_vma=False
    )
```

```python
import jax
import jax.numpy as jnp
from jax import lax
from jax.experimental import pallas as pl
from jax.experimental.pallas import tpu as pltpu
from jax.sharding import PartitionSpec as P

epsilon = 1e-06


def shifted(shard, axis, by):
    devices = lax.axis_size(axis)
    pairs = [(i, i + by) for i in range(devices) if 0 <= i + by < devices]
    return lax.ppermute(shard, axis, pairs)


def rms_norm(vector, gain):
    return vector * lax.rsqrt(jnp.mean(vector * vector, axis=-1, keepdims=True) + epsilon) * gain


def ring_order(count):
    return list(range(0, count, 2)) + list(range(count - 1, 0, -2))


def swapped(shard, axis, flip):
    devices = lax.axis_size(axis)
    return lax.ppermute(shard, axis, [(i, i ^ flip) for i in range(devices)])


def scatter_sum(partial, axis, cuts):
    devices = lax.axis_size(axis)
    blocks = partial.reshape(devices, partial.shape[0] // devices, partial.shape[1])
    index = lax.axis_index(axis)
    flip = 1
    while True:
        pairs = blocks.reshape(blocks.shape[0] // 2, 2, *blocks.shape[1:])
        mine = (index // flip) % 2
        low, high = pairs[:, 0], pairs[:, 1]
        keep = jnp.where(mine == 0, low, high)
        give = jnp.where(mine == 0, high, low).astype(jnp.bfloat16)
        if flip * 2 == devices:
            break
        blocks = keep.astype(jnp.float32) + swapped(give, axis, flip).astype(jnp.float32)
        flip *= 2
    size = keep.shape[1] // cuts
    halves = [slice(i * size, (i + 1) * size) for i in range(cuts)]
    gives = [give[0, part] for part in halves]
    return [(keep[0, part], swapped(g, axis, flip)) for part, g in zip(halves, gives)], gives


def scaled(vector, gain):
    return vector * lax.rsqrt(jnp.mean(vector * vector, axis=-1, keepdims=True) + epsilon) * gain


def norm_kernel(keep, got, resid, post_gain, pre_gain, stream, normed):
    projected = keep[...] + got[...].astype(jnp.float32)
    rows = (resid[...].astype(jnp.float32) + scaled(projected, post_gain[...])).astype(jnp.bfloat16)
    stream[...] = rows
    normed[...] = scaled(rows.astype(jnp.float32), pre_gain[...]).astype(jnp.bfloat16)


def norm_rows(keep, got, resid, post_gain, pre_gain, place):
    size, width = keep.shape
    full = pl.BlockSpec((size, width), lambda i: (0, 0))
    gain = pl.BlockSpec((1, width), lambda i: (0, 0))
    shape = jax.ShapeDtypeStruct((size, width), jnp.bfloat16)
    return pl.pallas_call(
        norm_kernel,
        grid=(1,),
        in_specs=[full, full, pl.BlockSpec((size, width), lambda i: (place, 0)), gain, gain],
        out_specs=[full, full],
        out_shape=[shape, shape],
        compiler_params=pltpu.CompilerParams(vmem_limit_bytes=24 * 1024 * 1024),
        name="norm_rows",
    )(keep, got, resid, post_gain[None], pre_gain[None])


def expert_call(parts, picks, table, gate_w, up_w, down_w):
    count, size, width = len(parts), parts[0].shape[0], parts[0].shape[1]
    hidden_width = gate_w.shape[2]
    block = 128 if hidden_width % 128 == 0 else hidden_width
    steps = hidden_width // block

    def kernel(*refs):
        ins, (weights, gate, up, down) = refs[:count], refs[count : count + 4]
        outs, (total,) = refs[count + 4 : 2 * count + 4], refs[2 * count + 4 :]
        rows = jnp.concatenate([ref[...] for ref in ins], axis=0)
        for step in range(steps):
            span = slice(step * block, (step + 1) * block)
            gate_pre = jnp.dot(rows, gate[0, :, span], preferred_element_type=jnp.float32)
            up_pre = jnp.dot(rows, up[0, :, span], preferred_element_type=jnp.float32)
            gate_act = jnp.minimum(gate_pre, 7.0)
            up_act = jnp.clip(up_pre, -7.0, 7.0)
            hidden = gate_act * jax.nn.sigmoid(1.702 * gate_act) * (up_act + 1.0)
            total[:, span] = hidden.astype(jnp.bfloat16)
        for i, (first, column) in enumerate(picks):
            weight = weights[first : first + size, column : column + 1]
            part = total[i * size : (i + 1) * size, :]
            out = jnp.dot(part, down[0], preferred_element_type=jnp.float32)
            outs[i][...] = (out * weight).astype(jnp.bfloat16)

    vmem = pl.BlockSpec(memory_space=pltpu.VMEM)
    held = [pltpu.with_memory_space_constraint(w, pltpu.VMEM) for w in (gate_w, up_w, down_w)]
    return pl.pallas_call(
        kernel,
        in_specs=[vmem] * (count + 4),
        out_specs=[vmem] * count,
        out_shape=[jax.ShapeDtypeStruct((size, width), jnp.bfloat16)] * count,
        scratch_shapes=[pltpu.VMEM((count * size, hidden_width), jnp.bfloat16)],
        cost_estimate=pl.CostEstimate(
            flops=6 * count * size * width * hidden_width,
            bytes_accessed=6 * width * hidden_width + 4 * count * size * width,
            transcendentals=count * size * hidden_width,
        ),
        compiler_params=pltpu.CompilerParams(vmem_limit_bytes=24 * 1024 * 1024),
        name="expert_rows",
    )(*parts, table, *held)


def finish_kernel(own_a, ahead_a, behind_a, own_b, ahead_b, behind_b, stream_a, stream_b, gain, out):
    size = own_a.shape[0]
    for i, (own, ahead, behind, stream) in enumerate(
        ((own_a, ahead_a, behind_a, stream_a), (own_b, ahead_b, behind_b, stream_b))
    ):
        combined = own[...].astype(jnp.float32) + ahead[...].astype(jnp.float32)
        combined = combined + behind[...].astype(jnp.float32)
        rows = stream[...].astype(jnp.float32) + scaled(combined, gain[...])
        out[i * size : (i + 1) * size, :] = rows.astype(jnp.bfloat16)


def finish(sums, streams, gain):
    size, width = streams[0].shape
    return pl.pallas_call(
        finish_kernel,
        out_shape=jax.ShapeDtypeStruct((2 * size, width), jnp.bfloat16),
        compiler_params=pltpu.CompilerParams(vmem_limit_bytes=24 * 1024 * 1024),
        name="finish",
    )(*sums[0], *sums[1], *streams, gain[None])


def joined(kept, got):
    return (kept.astype(jnp.float32) + got.astype(jnp.float32)).astype(jnp.bfloat16)


def tied(array, *others):
    return lax.optimization_barrier((array, *others))[0]


def ring_table(routes, route_weight, after):
    devices = lax.axis_size("sp")
    order = ring_order(devices)
    place_of = [order.index(i) for i in range(devices)]
    match = routes[:, :, None] == jnp.arange(devices, dtype=jnp.int32)[None, None, :]
    dense = jnp.sum(jnp.where(match, route_weight[:, :, None], 0.0), axis=1)
    table = lax.all_to_all(tied(dense, *after).T, "sp", split_axis=0, concat_axis=0, tiled=True)
    place = jnp.asarray(place_of, jnp.int32)[lax.axis_index("sp")]
    around = jnp.asarray(order, jnp.int32)[(place + jnp.arange(devices, dtype=jnp.int32)) % devices]
    return table[around].T


def ring_experts(halves, table, gate_w, up_w, down_w):
    devices = lax.axis_size("sp")
    size = halves[0].shape[0]
    order = ring_order(devices)
    ahead = [(order[i], order[(i + 1) % devices]) for i in range(devices)]
    behind = [(order[(i + 1) % devices], order[i]) for i in range(devices)]
    far = devices // 2

    def run(parts, picks):
        return expert_call(parts, picks, table, gate_w, up_w, down_w)

    forth, back = list(halves), list(halves)
    own = run(halves, [(0, 0), (size, 0)])
    kept_up, kept_down = {}, {}
    done = {1: [], 2: own}
    for step in range(1, far):
        for h in (0, 1):
            forth[h] = lax.ppermute(tied(forth[h], *done[step]), "sp", ahead)
            back[h] = lax.ppermute(tied(back[h], *done[step]), "sp", behind)
        out = run(
            [forth[0], forth[1], back[0], back[1]],
            [(0, devices - step), (size, devices - step), (0, step), (size, step)],
        )
        done[step + 2] = out
        kept_down[step], kept_up[step] = out[:2], out[2:]
    first = lax.ppermute(forth[0], "sp", ahead)
    last = lax.ppermute(back[1], "sp", behind)
    far_out = run([first, last], [(0, far), (size, far)])
    up = [lax.ppermute(far_out[0], "sp", ahead), None]
    down = [None, lax.ppermute(far_out[1], "sp", behind)]
    for step in range(far - 1, 0, -1):
        for h in (0, 1):
            up_rows = kept_up[step][h] if up[h] is None else joined(kept_up[step][h], up[h])
            down_rows = kept_down[step][h] if down[h] is None else joined(kept_down[step][h], down[h])
            up[h] = lax.ppermute(up_rows, "sp", ahead)
            down[h] = lax.ppermute(down_rows, "sp", behind)
    return [(own[h], up[h], down[h]) for h in (0, 1)]


def exchange_experts(normed, routes, route_weight, gate_w, up_w, down_w):
    own_count = normed.shape[0]
    width = normed.shape[1]
    top_count = routes.shape[1]
    experts = lax.axis_size("sp")
    capacity = 2 * own_count * top_count // experts
    flat_ids = routes.reshape(-1)
    assigned = flat_ids.shape[0]
    onehot = (flat_ids[:, None] == jnp.arange(experts, dtype=jnp.int32)[None, :]).astype(jnp.int32)
    earlier = jnp.cumsum(onehot, axis=0) - onehot
    slot_index = jnp.sum(earlier * onehot, axis=1)
    target = flat_ids * capacity + slot_index
    source = (
        jnp.full((experts * capacity,), assigned, jnp.int32)
        .at[target]
        .set(jnp.arange(assigned, dtype=jnp.int32))
    )
    row_index = jnp.where(source < assigned, source // top_count, own_count)
    with_blank = jnp.concatenate([normed, jnp.zeros((1, width), jnp.bfloat16)], axis=0)
    outgoing = with_blank[row_index].reshape(experts, capacity, width)
    slots_in = lax.all_to_all(outgoing, "sp", split_axis=0, concat_axis=0, tiled=True)
    gate_pre = jnp.dot(slots_in, gate_w[0], preferred_element_type=jnp.float32)
    up_pre = jnp.dot(slots_in, up_w[0], preferred_element_type=jnp.float32)
    gate_act = jnp.minimum(gate_pre, 7.0)
    up_act = jnp.clip(up_pre, -7.0, 7.0)
    hidden = (gate_act * jax.nn.sigmoid(1.702 * gate_act) * (up_act + 1.0)).astype(jnp.bfloat16)
    expert_out = jnp.dot(hidden, down_w[0], preferred_element_type=jnp.float32).astype(jnp.bfloat16)
    returned = lax.all_to_all(expert_out, "sp", split_axis=0, concat_axis=0, tiled=True)
    chosen = returned.reshape(experts * capacity, width)[target].astype(jnp.float32)
    weighted = chosen * route_weight.reshape(-1)[:, None]
    return jnp.sum(weighted.reshape(own_count, top_count, width), axis=1)


def body(
    b_gate,
    c_gate,
    values_in,
    conv_taps,
    out_proj,
    resid,
    post_gain,
    pre_gain,
    moe_gain,
    routes,
    route_weight,
    gate_w,
    up_w,
    down_w,
):
    tok_rows = b_gate.shape[0]
    product = c_gate.astype(jnp.float32) * values_in.astype(jnp.float32)
    prior_rows = shifted(product[tok_rows - 2 :], "sp", 1)
    padded = jnp.concatenate([prior_rows, product], axis=0)
    filtered = (
        padded[0:tok_rows] * conv_taps[0]
        + padded[1 : tok_rows + 1] * conv_taps[1]
        + padded[2 : tok_rows + 2] * conv_taps[2]
    )
    mixed_rows = (b_gate.astype(jnp.float32) * filtered).astype(jnp.bfloat16)
    partial = jnp.dot(mixed_rows, out_proj, preferred_element_type=jnp.float32).astype(jnp.bfloat16)
    pairs, given = scatter_sum(partial, "tp", 2)
    spread = lax.axis_size("sp") * routes.shape[0]
    ring = 2 * routes.shape[0] * routes.shape[1] >= spread
    table = ring_table(routes, route_weight, given) if ring else None
    streams, normed = [], []
    for place, (keep, got) in enumerate(pairs):
        keep = tied(keep, table) if ring and place == 1 else keep
        rows = norm_rows(keep, got, resid, post_gain, pre_gain, place)
        streams.append(rows[0])
        normed.append(rows[1])
    if ring:
        sums = ring_experts(normed, table, gate_w, up_w, down_w)
        return finish(sums, streams, moe_gain)
    stream = jnp.concatenate(streams, axis=0)
    normed = jnp.concatenate(normed, axis=0)
    combined = exchange_experts(normed, routes, route_weight, gate_w, up_w, down_w)
    return (stream.astype(jnp.float32) + rms_norm(combined, moe_gain)).astype(jnp.bfloat16)


def solution(mesh):
    placed = (
        P("sp", "tp"),
        P("sp", "tp"),
        P("sp", "tp"),
        P(None, "tp"),
        P("tp", None),
        P(("sp", "tp"), None),
        P(),
        P(),
        P(),
        P(("sp", "tp"), None),
        P(("sp", "tp"), None),
        P("sp", None, None),
        P("sp", None, None),
        P("sp", None, None),
    )
    return jax.shard_map(
        body, mesh=mesh, in_specs=placed, out_specs=P(("sp", "tp"), None), check_vma=False
    )
```
